32 devices in a mesh: ep: 8 (over z, y), tp: 4 (over x, core).
Axes of the slice: x: 2, y: 2, z: 4, core: 2. Of those that a mesh axis runs over, the one named last changes fastest.
Arguments:
- tokens: bfloat16 [1024, 2048], P('ep', 'tp'), may hold values from -6 to 6
- norm_gain: bfloat16 [2048], P('tp'), may hold values from 0.099609375 to 1.8984375
- routes: int32 [1024, 2], P('ep'), may hold values from 0 to 7, as said below
- gate_weights: float32 [1024, 2], P('ep'), may hold values from 0.1 to 1
- w_gate: bfloat16 [8, 2048, 4096], P('ep', None, 'tp'), may hold values from -0.125 to 0.125
- w_up: bfloat16 [8, 2048, 4096], P('ep', None, 'tp'), may hold values from -0.125 to 0.125
- w_down: bfloat16 [8, 4096, 2048], P('ep', 'tp'), may hold values from -0.875 to 0.875
- out_gain: bfloat16 [2048], P('tp'), may hold values from 0.099609375 to 1.8984375
Outputs:
- mixed: bfloat16 [1024, 2048], P('ep', 'tp')
The draws below stay inside these ranges and needn't reach their ends.
Inputs may be any that keep to these rules, and one draw needn't show every extreme that they name: `routes`: each row names 2 different experts of one group (their quotients by 8 agree). In each aligned block of 128 rows no expert is named by more than 64 rows, and in every block some expert is named by exactly 64 rows.
All inputs are finite; a program needn't handle non-finite values.
Results may differ from the reference program's by a relative error of at most 0.019.
Values may be sent and summed in bfloat16 or wider, within the bound.
A program may use at most 64 MiB of HBM per device.

```python
import math
import jax
import jax.numpy as jnp
from jax import lax

D = 2048
FF = 4096
EPG = 8
TOPK = 2
TOK_DEV = 128
EXPERTS = 8
GROUPS = 1
MEAN = 32
CAP = 64
TOKENS = 1024
N_EP = 8
N_TP = 4


def draw_routes(key, part):
    folded = jax.random.fold_in(key, 5)
    k_pop, k_jit, k_perm = jax.random.split(folded, 3)
    popular = jax.random.randint(k_pop, (EXPERTS,), 0, 4)
    jitter = jax.random.randint(k_jit, (N_EP, EXPERTS), 0, 3)
    expert_ids = jnp.arange(EXPERTS, dtype=jnp.int32)
    scores = (popular[None, :] * 4 + jitter) * EXPERTS + expert_ids[None, :]
    sorted_ids = jnp.argsort(scores, axis=1)
    ranking = jnp.argsort(sorted_ids, axis=1)
    quarter = ranking * 4 // EXPERTS
    counts = jnp.where(quarter == 3, 2 * MEAN, jnp.where(quarter == 2, MEAN, MEAN // 2)).astype(jnp.int32)
    group_copies = counts.reshape(N_EP, GROUPS, EPG).sum(axis=2)
    group_tokens = group_copies // 2
    token_end = jnp.cumsum(group_tokens, axis=1)
    token_start = token_end - group_tokens
    copy_start = jnp.cumsum(group_copies, axis=1) - group_copies
    expert_end = jnp.cumsum(counts, axis=1)
    positions = jnp.arange(TOK_DEV, dtype=jnp.int32)
    group_of = jnp.sum(positions[None, :, None] >= token_end[:, None, :], axis=2).astype(jnp.int32)
    within = positions[None, :] - jnp.take_along_axis(token_start, group_of, axis=1)
    first_copy = jnp.take_along_axis(copy_start, group_of, axis=1) + within
    second_copy = first_copy + jnp.take_along_axis(group_tokens, group_of, axis=1)

    def owner_of(copies):
        return jnp.sum(copies[:, :, None] >= expert_end[:, None, :], axis=2).astype(jnp.int32)
    chosen = jnp.stack([owner_of(first_copy), owner_of(second_copy)], axis=2)
    shuffle = jax.random.randint(k_perm, (N_EP, TOK_DEV), 0, 1 << 20) * TOK_DEV + positions[None, :]
    shuffled_order = jnp.argsort(shuffle, axis=1)
    chosen = jnp.take_along_axis(chosen, shuffled_order[:, :, None], axis=1)
    return chosen.reshape(N_EP * TOK_DEV, 2).astype(jnp.int32)


def draw_w_down(key, part):
    k_base, k_rough = jax.random.split(jax.random.fold_in(key, 7))
    column = jnp.arange(D, dtype=jnp.float32) / D
    base = jnp.clip(jax.random.normal(k_base, (EXPERTS, FF, D), jnp.float32), -4.0, 4.0)
    rising = 10.0 ** column
    rough = jax.random.uniform(k_rough, (D,), jnp.float32, 0.6, 1.4)
    return (base * (rising * rough / FF ** 0.5)[None, None, :]).astype(jnp.bfloat16)


def block_levels(own_key, shape, pieces, least, largest):
    def one(axis_at, parts):
        draws = jax.random.uniform(jax.random.fold_in(jax.random.fold_in(own_key, 6), axis_at), (parts,), jnp.float32, least / len(pieces), largest / len(pieces))
        return jnp.repeat(jnp.exp(draws), shape[axis_at] // parts).reshape((-1,) + (1,) * (len(shape) - axis_at - 1))

    gain = one(*pieces[0])
    for cut in pieces[1:]:
        gain = gain * one(*cut)
    return gain


def bell_draw(rng, extent, width, limit, shards=(), held_as=jnp.bfloat16):
    factor_of = block_levels(rng, extent, shards, -0.22, 0.18) if shards else 1.0
    result = jax.random.normal(rng, extent, jnp.float32) * width * factor_of
    return jnp.minimum(jnp.maximum(result, -limit), limit).astype(held_as)


def setup_inputs(seed: int = 0) -> dict:
    keys = jax.random.split(jax.random.key(seed), 9)
    tokens = bell_draw(keys[0], (TOKENS, D), 1.0, 6.0, ((0, 8), (1, 4)))
    norm_gain = jnp.clip(1.0 + 0.18 * jax.random.normal(keys[1], (D,), jnp.float32), 0.099609375, 1.8984375).astype(jnp.bfloat16)
    routes = draw_routes(jax.random.fold_in(keys[8], 71), 0)
    gate_weights = jnp.clip(jnp.exp(math.log(1.0) - 2.3025851 * jax.random.uniform(keys[3], (TOKENS, TOPK), jnp.float32) ** block_levels(keys[3], (TOKENS, TOPK), ((0, 8),), -0.2, 0.2)), 0.1, 1.0)
    w_gate = bell_draw(keys[4], (EXPERTS, D, FF), D ** -0.5, 0.125, ((0, 8), (2, 4)))
    w_up = bell_draw(keys[5], (EXPERTS, D, FF), D ** -0.5, 0.125, ((0, 8), (2, 4)))
    w_down = draw_w_down(jax.random.fold_in(keys[8], 71), 0)
    out_gain = jnp.clip(1.0 + 0.18 * jax.random.normal(keys[7], (D,), jnp.float32), 0.099609375, 1.8984375).astype(jnp.bfloat16)
    return dict(tokens=tokens, norm_gain=norm_gain, routes=routes, gate_weights=gate_weights, w_gate=w_gate, w_up=w_up, w_down=w_down, out_gain=out_gain)


epsilon = 1e-06

def route_slots(routes):
    blocks = routes.reshape(N_EP, TOK_DEV * TOPK)
    onehot = (blocks[:, :, None] == jnp.arange(EXPERTS, dtype=jnp.int32)[None, None, :]).astype(jnp.int32)
    before = jnp.cumsum(onehot, axis=1) - onehot
    return lax.optimization_barrier(jnp.sum(before * onehot, axis=2)).astype(jnp.int32)

def reference(tokens, norm_gain, routes, gate_weights, w_gate, w_up, w_down, out_gain):
    x_float = tokens.astype(jnp.float32)
    scale_in = lax.rsqrt(lax.optimization_barrier(jnp.mean(x_float * x_float, axis=1, keepdims=True)) + epsilon)
    normed = (x_float * scale_in * norm_gain.astype(jnp.float32)).astype(jnp.bfloat16)
    slot_index = route_slots(routes)
    expert_ids = routes.reshape(N_EP, TOK_DEV * TOPK).astype(jnp.int32)
    source = jnp.arange(N_EP, dtype=jnp.int32)[:, None]
    copy_ids = jnp.arange(TOK_DEV * TOPK, dtype=jnp.int32)[None, :]
    token_ids = (source * TOK_DEV + copy_ids // TOPK).astype(jnp.int32)
    buffer_pos = (source * CAP + slot_index).astype(jnp.int32)
    table = jnp.full((EXPERTS, N_EP * CAP), TOKENS, jnp.int32).at[expert_ids, buffer_pos].set(token_ids)
    padded = jnp.concatenate([normed, jnp.zeros((1, D), jnp.bfloat16)], axis=0)

    def expert(inputs):
        row_table, gate_mat, up_mat, down_mat = inputs
        arrived = padded[row_table]
        gate_sum = jnp.dot(arrived, gate_mat, preferred_element_type=jnp.float32)
        up_sum = jnp.dot(arrived, up_mat, preferred_element_type=jnp.float32)
        hidden = (jax.nn.silu(gate_sum) * up_sum).astype(jnp.bfloat16)
        hidden_blocks = hidden.reshape(N_EP * CAP, N_TP, FF // N_TP).astype(jnp.float32)
        down_blocks = down_mat.reshape(N_TP, FF // N_TP, D).astype(jnp.float32)
        partial_value = jnp.einsum('rtf,tfd->trd', hidden_blocks, down_blocks).astype(jnp.bfloat16)
        partial_value = lax.optimization_barrier(partial_value)
        return lax.optimization_barrier(jnp.sum(partial_value.astype(jnp.float32), axis=0)).astype(jnp.bfloat16)
    outputs = lax.map(expert, (table, w_gate, w_up, w_down))
    picked = outputs[expert_ids, buffer_pos].astype(jnp.float32).reshape(TOKENS, TOPK, D)
    combined = lax.optimization_barrier(jnp.sum(picked * gate_weights[:, :, None], axis=1))
    scale_out = lax.rsqrt(lax.optimization_barrier(jnp.mean(combined * combined, axis=1, keepdims=True)) + epsilon)
    return (combined * scale_out * out_gain.astype(jnp.float32)).astype(jnp.bfloat16)
```

```python
import functools

import jax
import jax.numpy as jnp
from jax import lax
from jax.experimental import pallas as pl
from jax.experimental.pallas import tpu as pltpu
from jax.sharding import PartitionSpec as P

epsilon = 1e-06
CORES = 2


def shards(tokens, norm_gain, routes, gate_weights, w_gate, w_up, w_down, out_gain):
    tok_rows = tokens.shape[0]
    width_local = tokens.shape[1]
    full_width = width_local * lax.axis_size("tp")
    experts = lax.axis_size("ep")
    top_count = routes.shape[1]
    capacity = 2 * top_count * tok_rows // experts
    flat_ids = routes.reshape(-1)
    onehot = (flat_ids[:, None] == jnp.arange(experts, dtype=jnp.int32)[None, :]).astype(jnp.int32)
    before = jnp.cumsum(onehot, axis=0) - onehot
    slot_index = jnp.sum(before * onehot, axis=1)
    dest_index = flat_ids * capacity + slot_index
    dest_pairs = dest_index.reshape(tok_rows, top_count)
    places = jnp.arange(experts * capacity, dtype=jnp.int32)
    scatter_mat = jnp.any(dest_pairs[None, :, :] == places[:, None, None], axis=2).astype(
        jnp.bfloat16
    )
    gate_mat = w_gate[0]
    up_mat = w_up[0]
    x_float = tokens.astype(jnp.float32)
    row_sums = lax.psum(jnp.sum(x_float * x_float, axis=1), "tp")
    scale_in = lax.rsqrt(row_sums / full_width + epsilon)
    normed = (x_float * scale_in[:, None] * norm_gain.astype(jnp.float32)).astype(jnp.bfloat16)
    outgoing = jnp.dot(scatter_mat, normed, preferred_element_type=jnp.float32).astype(jnp.bfloat16)
    arrived = lax.all_to_all(outgoing, "ep", split_axis=0, concat_axis=0, tiled=True)
    portion = lax.all_gather(arrived, "tp", axis=1, tiled=True)
    gate_sum = jnp.dot(portion, gate_mat, preferred_element_type=jnp.float32)
    up_sum = jnp.dot(portion, up_mat, preferred_element_type=jnp.float32)
    hidden = (jax.nn.silu(gate_sum) * up_sum).astype(jnp.bfloat16)
    down_mat = w_down[0]
    summed = lax.psum_scatter(
        lax.dot_general(
            down_mat, hidden, (((0,), (1,)), ((), ())), preferred_element_type=jnp.float32
        ).astype(jnp.bfloat16),
        "tp",
        scatter_dimension=0,
        tiled=True,
    )
    came_back = lax.all_to_all(summed, "ep", split_axis=1, concat_axis=1, tiled=True)
    picked = (
        jnp.take(came_back, dest_index, axis=1)
        .astype(jnp.float32)
        .reshape(width_local, tok_rows, top_count)
    )
    combined = jnp.sum(picked * gate_weights[None, :, :], axis=2).T
    out_sums = lax.psum(jnp.sum(combined * combined, axis=1), "tp")
    scale_out = lax.rsqrt(out_sums / full_width + epsilon)
    return (combined * scale_out[:, None] * out_gain.astype(jnp.float32)).astype(jnp.bfloat16)


def xor(index, mask):
    result = index
    bit = 1
    while bit <= mask:
        if mask & bit:
            result = result + bit * (1 - 2 * ((index // bit) % 2))
        bit *= 2
    return result


def layer(
    n_ep, cap, near,
    routes_ref, gates_ref, tokens_ref, in_gain_ref, out_gain_ref, wg_hbm, wu_hbm, wd_hbm,
    out_ref,
    wg, wu, wd, picked, xall, gains, xn, hidden, psend, prec, own, xsend, xrec, rsend, back, sums,
    w_sem, disp_s, disp_r, part_s, part_r, opp_s, opp_r, rel_s, rel_r, gain_s, gain_r,
    pd_s, pd_r, xs_s, xs_r, ret_s, ret_r, ns_s, ns_r,
):
    f32, bf16 = jnp.float32, jnp.bfloat16
    ep, tp = lax.axis_index("ep"), lax.axis_index("tp")
    chip, core = tp // CORES, tp % CORES
    partner = chip * CORES + (1 - core)
    opposite = (1 - chip) * CORES + core
    diagonal = (1 - chip) * CORES + (1 - core)
    tok, width = tokens_ref.shape
    n_tp = gains.shape[0]
    full = width * n_tp
    ff = wg.shape[1]
    half_rows = n_ep // 2 * cap
    source = [xor(ep, d) for d in range(n_ep)]
    rows = [pl.ds(pl.multiple_of(s * cap, cap), cap) for s in source]
    my_rows = rows[0]

    barrier = pltpu.get_barrier_semaphore()
    for d in range(1, n_ep):
        pl.semaphore_signal(barrier, inc=1, device_id={"ep": source[d]})
    for peer in (partner, opposite, diagonal):
        pl.semaphore_signal(barrier, inc=1, device_id={"tp": peer})

    weights = [
        pltpu.make_async_copy(src.at[0], dst, w_sem.at[i])
        for i, (src, dst) in enumerate(((wg_hbm, wg), (wu_hbm, wu), (wd_hbm, wd)))
    ]
    for copy in weights:
        copy.start()

    def remote(src, dst, send, recv, where):
        return pltpu.make_async_remote_copy(
            src_ref=src, dst_ref=dst, send_sem=send, recv_sem=recv, device_id=where
        )

    routes = routes_ref[...]
    first, second = routes[:, 0:1], routes[:, 1:2]
    lanes = 128 * pl.cdiv(n_ep, 128)
    expert = lax.broadcasted_iota(jnp.int32, (tok, lanes), 1)
    is_first, is_second = expert == first, expert == second
    member = jnp.where(is_first, 1.0, 0.0) + jnp.where(is_second, 1.0, 0.0)
    earlier = jnp.where(
        lax.broadcasted_iota(jnp.int32, (tok, tok), 1)
        < lax.broadcasted_iota(jnp.int32, (tok, tok), 0),
        1.0,
        0.0,
    )
    before = jnp.dot(earlier.astype(bf16), member.astype(bf16), preferred_element_type=f32)
    place = before + (expert * cap).astype(f32)
    place_first = jnp.sum(jnp.where(is_first, place, 0.0), axis=1, keepdims=True)
    place_second = jnp.sum(jnp.where(is_second, place, 0.0), axis=1, keepdims=True)
    slots = lax.broadcasted_iota(jnp.int32, (tok, n_ep * cap), 1).astype(f32)
    at_first, at_second = slots == place_first, slots == place_second
    select = (jnp.where(at_first, 1.0, 0.0) + jnp.where(at_second, 1.0, 0.0)).astype(bf16)
    picked[...] = lax.dot_general(
        select, tokens_ref[...], (((0,), (0,)), ((), ())), preferred_element_type=f32
    ).astype(bf16)
    gains[pl.ds(tp, 1)] = in_gain_ref[...].astype(f32)[None]
    xall[pl.ds(tp, 1), my_rows] = picked[my_rows][None]

    pl.semaphore_wait(barrier, n_ep - 1 + n_tp - 1)

    dispatch = {
        d: remote(picked.at[rows[d]], xall.at[tp, my_rows], disp_s.at[d], disp_r.at[d], {"ep": source[d]})
        for d in range(1, n_ep)
    }
    to_partner, to_opposite, relay = [], [], []
    for d in range(n_ep):
        block = xall.at[tp, rows[d]]
        to_partner.append(remote(block, block, part_s.at[d], part_r.at[d], {"tp": partner}))
        to_opposite.append(remote(block, block, opp_s.at[d], opp_r.at[d], {"tp": opposite}))
        far = xall.at[opposite, rows[d]]
        relay.append(remote(far, far, rel_s.at[d], rel_r.at[d], {"tp": partner}))
    gain_copies = [
        remote(gains.at[tp], gains.at[tp], gain_s.at[i], gain_r.at[i], {"tp": peer})
        for i, peer in enumerate((partner, opposite, diagonal))
    ]
    for copy in gain_copies:
        copy.start()
    to_opposite[0].start()
    to_partner[0].start()
    order = near[1:]
    for d in order:
        dispatch[d].start()

    def forward(d):
        dispatch[d].wait_recv()
        to_opposite[d].start()
        to_partner[d].start()

    def pass_on(d):
        to_opposite[d].wait_recv()
        relay[d].start()

    def normalise(i, d):
        to_partner[d].wait_recv()
        relay[d].wait_recv()
        parts = [xall[j, rows[d]].astype(f32) for j in range(n_tp)]
        total = sum(jnp.sum(p * p, axis=1, keepdims=True) for p in parts)
        scale = lax.rsqrt(total / full + epsilon)
        for j in range(n_tp):
            xn[i * cap : (i + 1) * cap, j * width : (j + 1) * width] = (
                parts[j] * scale * gains[j]
            ).astype(bf16)

    tile = min(256, ff)
    tiles = ff // tile

    def units(h, start, stop):
        mine = slice(h * half_rows, (h + 1) * half_rows)

        def body(n, carry):
            cols = pl.ds(pl.multiple_of(n * tile, tile), tile)
            gate = jnp.dot(xn[mine], wg[:, cols], preferred_element_type=f32)
            up = jnp.dot(xn[mine], wu[:, cols], preferred_element_type=f32)
            hidden[mine, cols] = (gate / (1.0 + jnp.exp(-gate)) * up).astype(bf16)
            return carry

        lax.fori_loop(start, stop, body, 0)

    far_partner, near_partner = diagonal, partner
    partner_copies = {
        (h, k): remote(psend.at[h, k], prec.at[h, k], pd_s.at[h, k], pd_r.at[h, k], {"tp": partner})
        for h in range(2)
        for k in range(2)
    }

    def down(h):
        mine = slice(h * half_rows, (h + 1) * half_rows)

        def product(j):
            cols = pl.ds(pl.multiple_of(j * width, width), width)
            return jnp.dot(hidden[mine], wd[:, cols], preferred_element_type=f32)

        for k, j in enumerate((far_partner, near_partner)):
            psend[h, k] = product(j).astype(bf16)
            partner_copies[h, k].start()
        for k, j in enumerate((opposite, tp)):
            own[h, k] = product(j)

    across = [
        remote(xsend.at[i], xrec.at[i], xs_s.at[i], xs_r.at[i], {"tp": opposite})
        for i in range(n_ep)
    ]
    returned = {
        d: remote(rsend.at[d], back.at[my_rows], ret_s.at[d], ret_r.at[d], {"ep": source[d]})
        for d in range(1, n_ep)
    }

    def send_across(h):
        partner_copies[h, 0].wait_recv()
        for q in range(n_ep // 2):
            i = h * (n_ep // 2) + q
            part = slice(q * cap, (q + 1) * cap)
            xsend[i] = (own[h, 0, part] + prec[h, 0, part].astype(f32)).astype(bf16)
            across[i].start()

    def send_back(h):
        partner_copies[h, 1].wait_recv()
        for q in range(n_ep // 2):
            i = h * (n_ep // 2) + q
            d = near[i]
            part = slice(q * cap, (q + 1) * cap)
            both = own[h, 1, part] + prec[h, 1, part].astype(f32)
            across[i].wait_recv()
            done = (both + xrec[i].astype(f32)).astype(bf16)
            if d == 0:
                back[my_rows] = done
            else:
                rsend[d] = done
                returned[d].start()

    half = n_ep // 2
    group_a, group_b = near[:half], near[half:]
    for copy in gain_copies:
        copy.wait_recv()
    for i in range(1, half):
        forward(group_a[i])
        pass_on(group_a[i - 1])
    pass_on(group_a[half - 1])
    for i, d in enumerate(group_a):
        normalise(i, d)
    for copy in weights[:2]:
        copy.wait()
    pieces = min(half, tiles)
    done = 0
    for piece in range(pieces):
        until = (piece + 1) * half // pieces
        for i in range(done, until):
            forward(group_b[i])
            if i:
                pass_on(group_b[i - 1])
        done = until
        units(0, piece * tiles // pieces, (piece + 1) * tiles // pieces)
    pass_on(group_b[half - 1])
    weights[2].wait()
    down(0)
    send_across(0)
    for i, d in enumerate(group_b):
        normalise(half + i, d)
    units(1, 0, tiles)
    send_back(0)
    down(1)
    send_across(1)
    send_back(1)

    gates = gates_ref[...]
    mixing = jnp.where(at_first, gates[:, 0:1], 0.0) + jnp.where(at_second, gates[:, 1:2], 0.0)
    high = mixing.astype(bf16)
    low = (mixing - high.astype(f32)).astype(bf16)
    for d in range(1, n_ep):
        returned[d].wait_recv()
    rows_back = back[...]
    combined = jnp.dot(high, rows_back, preferred_element_type=f32) + jnp.dot(
        low, rows_back, preferred_element_type=f32
    )
    diag = lax.broadcasted_iota(jnp.int32, (tok, tok), 0) == lax.broadcasted_iota(
        jnp.int32, (tok, tok), 1
    )
    row_sum = jnp.sum(combined * combined, axis=1, keepdims=True)
    flat = jnp.sum(jnp.where(diag, row_sum, 0.0), axis=0, keepdims=True)
    sums[pl.ds(tp, 1)] = flat[None]
    norm_copies = [
        remote(sums.at[tp], sums.at[tp], ns_s.at[i], ns_r.at[i], {"tp": peer})
        for i, peer in enumerate((partner, opposite, diagonal))
    ]
    for copy in norm_copies:
        copy.start()

    for copy in gain_copies + to_partner + to_opposite + relay + across:
        copy.wait_send()
    for copies in (dispatch, partner_copies, returned):
        for copy in copies.values():
            copy.wait_send()

    for copy in norm_copies:
        copy.wait()
    total = sum(sums[j] for j in range(n_tp))
    column = jnp.sum(jnp.where(diag, total, 0.0), axis=1, keepdims=True)
    scale = lax.rsqrt(column / full + epsilon)
    out_ref[...] = (combined * scale * out_gain_ref[...].astype(f32)).astype(bf16)


def fused(tokens, norm_gain, routes, gate_weights, w_gate, w_up, w_down, out_gain):
    n_ep, n_tp = lax.axis_size("ep"), lax.axis_size("tp")
    tok, width = tokens.shape
    cap = 2 * routes.shape[1] * tok // n_ep
    _, d_model, ff = w_gate.shape
    half_rows = n_ep // 2 * cap
    near = (0, 2, 3, 1) + tuple(range(4, n_ep))
    bf16, f32 = jnp.bfloat16, jnp.float32
    dma = pltpu.SemaphoreType.DMA
    vmem = pl.BlockSpec(memory_space=pltpu.VMEM)
    anywhere = pl.BlockSpec(memory_space=pl.ANY)
    slots = n_ep * cap
    return pl.pallas_call(
        functools.partial(layer, n_ep, cap, near),
        out_shape=jax.ShapeDtypeStruct((tok, width), bf16),
        in_specs=[vmem] * 5 + [anywhere] * 3,
        out_specs=vmem,
        scratch_shapes=[
            pltpu.VMEM((d_model, ff), bf16),
            pltpu.VMEM((d_model, ff), bf16),
            pltpu.VMEM((ff, d_model), bf16),
            pltpu.VMEM((slots, width), bf16),
            pltpu.VMEM((n_tp, slots, width), bf16),
            pltpu.VMEM((n_tp, 1, width), f32),
            pltpu.VMEM((slots, d_model), bf16),
            pltpu.VMEM((slots, ff), bf16),
            pltpu.VMEM((2, 2, half_rows, width), bf16),
            pltpu.VMEM((2, 2, half_rows, width), bf16),
            pltpu.VMEM((2, 2, half_rows, width), f32),
            pltpu.VMEM((n_ep, cap, width), bf16),
            pltpu.VMEM((n_ep, cap, width), bf16),
            pltpu.VMEM((n_ep, cap, width), bf16),
            pltpu.VMEM((slots, width), bf16),
            pltpu.VMEM((n_tp, 1, tok), f32),
            dma((3,)),
            *[dma((n_ep,))] * 8,
            *[dma((3,))] * 2,
            *[dma((2, 2))] * 2,
            *[dma((n_ep,))] * 4,
            *[dma((3,))] * 2,
        ],
        compiler_params=pltpu.CompilerParams(
            collective_id=0, has_side_effects=True, vmem_limit_bytes=60 * 1024 * 1024
        ),
    )(
        routes, gate_weights, tokens, norm_gain.reshape(1, -1), out_gain.reshape(1, -1),
        w_gate, w_up, w_down,
    )


def solution(mesh):
    placed = (
        P("ep", "tp"),
        P("tp"),
        P("ep", None),
        P("ep", None),
        P("ep", None, "tp"),
        P("ep", None, "tp"),
        P("ep", "tp", None),
        P("tp"),
    )
    n_ep = mesh.shape["ep"]
    pairs = mesh.shape["tp"] == 2 * CORES and n_ep >= 8 and n_ep & (n_ep - 1) == 0
    return jax.shard_map(
        fused if pairs else shards, mesh=mesh, in_specs=placed, out_specs=P("ep", "tp"), check_vma=False
    )
```

```python
import functools

import jax
import jax.numpy as jnp
from jax import lax
from jax.experimental import pallas as pl
from jax.experimental.pallas import tpu as pltpu
from jax.sharding import PartitionSpec as P

epsilon = 1e-06
CORES = 2


def shards(tokens, norm_gain, routes, gate_weights, w_gate, w_up, w_down, out_gain):
    tok_rows = tokens.shape[0]
    width_local = tokens.shape[1]
    full_width = width_local * lax.axis_size("tp")
    experts = lax.axis_size("ep")
    top_count = routes.shape[1]
    capacity = 2 * top_count * tok_rows // experts
    flat_ids = routes.reshape(-1)
    onehot = (flat_ids[:, None] == jnp.arange(experts, dtype=jnp.int32)[None, :]).astype(jnp.int32)
    before = jnp.cumsum(onehot, axis=0) - onehot
    slot_index = jnp.sum(before * onehot, axis=1)
    dest_index = flat_ids * capacity + slot_index
    dest_pairs = dest_index.reshape(tok_rows, top_count)
    places = jnp.arange(experts * capacity, dtype=jnp.int32)
    scatter_mat = jnp.any(dest_pairs[None, :, :] == places[:, None, None], axis=2).astype(
        jnp.bfloat16
    )
    gate_mat = w_gate[0]
    up_mat = w_up[0]
    x_float = tokens.astype(jnp.float32)
    row_sums = lax.psum(jnp.sum(x_float * x_float, axis=1), "tp")
    scale_in = lax.rsqrt(row_sums / full_width + epsilon)
    normed = (x_float * scale_in[:, None] * norm_gain.astype(jnp.float32)).astype(jnp.bfloat16)
    outgoing = jnp.dot(scatter_mat, normed, preferred_element_type=jnp.float32).astype(jnp.bfloat16)
    arrived = lax.all_to_all(outgoing, "ep", split_axis=0, concat_axis=0, tiled=True)
    portion = lax.all_gather(arrived, "tp", axis=1, tiled=True)
    gate_sum = jnp.dot(portion, gate_mat, preferred_element_type=jnp.float32)
    up_sum = jnp.dot(portion, up_mat, preferred_element_type=jnp.float32)
    hidden = (jax.nn.silu(gate_sum) * up_sum).astype(jnp.bfloat16)
    down_mat = w_down[0]
    summed = lax.psum_scatter(
        lax.dot_general(
            down_mat, hidden, (((0,), (1,)), ((), ())), preferred_element_type=jnp.float32
        ).astype(jnp.bfloat16),
        "tp",
        scatter_dimension=0,
        tiled=True,
    )
    came_back = lax.all_to_all(summed, "ep", split_axis=1, concat_axis=1, tiled=True)
    picked = (
        jnp.take(came_back, dest_index, axis=1)
        .astype(jnp.float32)
        .reshape(width_local, tok_rows, top_count)
    )
    combined = jnp.sum(picked * gate_weights[None, :, :], axis=2).T
    out_sums = lax.psum(jnp.sum(combined * combined, axis=1), "tp")
    scale_out = lax.rsqrt(out_sums / full_width + epsilon)
    return (combined * scale_out[:, None] * out_gain.astype(jnp.float32)).astype(jnp.bfloat16)


def xor(index, mask):
    result = index
    bit = 1
    while bit <= mask:
        if mask & bit:
            result = result + bit * (1 - 2 * ((index // bit) % 2))
        bit *= 2
    return result


def layer(
    n_ep, cap, near,
    routes_ref, gates_ref, tokens_ref, in_gain_ref, out_gain_ref, wg_hbm, wu_hbm, wd_hbm,
    out_ref,
    wg, wu, wd, picked, xall, gains, xn, hidden, psend, prec, own, xsend, xrec, rsend, back, sums,
    w_sem, disp_s, disp_r, part_s, part_r, opp_s, opp_r, rel_s, rel_r, gain_s, gain_r,
    pd_s, pd_r, xs_s, xs_r, ret_s, ret_r, ns_s, ns_r,
):
    f32, bf16 = jnp.float32, jnp.bfloat16
    ep, tp = lax.axis_index("ep"), lax.axis_index("tp")
    chip, core = tp // CORES, tp % CORES
    partner = chip * CORES + (1 - core)
    opposite = (1 - chip) * CORES + core
    diagonal = (1 - chip) * CORES + (1 - core)
    tok, width = tokens_ref.shape
    n_tp = gains.shape[0]
    full = width * n_tp
    ff = wg.shape[1]
    half_rows = n_ep // 2 * cap
    source = [xor(ep, d) for d in range(n_ep)]
    rows = [pl.ds(pl.multiple_of(s * cap, cap), cap) for s in source]
    my_rows = rows[0]

    barrier = pltpu.get_barrier_semaphore()
    for d in range(1, n_ep):
        pl.semaphore_signal(barrier, inc=1, device_id={"ep": source[d]})
    for peer in (partner, opposite, diagonal):
        pl.semaphore_signal(barrier, inc=1, device_id={"tp": peer})

    weights = [
        pltpu.make_async_copy(src.at[0], dst, w_sem.at[i])
        for i, (src, dst) in enumerate(((wg_hbm, wg), (wu_hbm, wu), (wd_hbm, wd)))
    ]
    for copy in weights:
        copy.start()

    def remote(src, dst, send, recv, where):
        return pltpu.make_async_remote_copy(
            src_ref=src, dst_ref=dst, send_sem=send, recv_sem=recv, device_id=where
        )

    diag = lax.broadcasted_iota(jnp.int32, (tok, tok), 0) == lax.broadcasted_iota(
        jnp.int32, (tok, tok), 1
    )

    def column(row):
        return jnp.sum(jnp.where(diag, row, 0.0), axis=1, keepdims=True)

    routes = routes_ref[...].astype(f32)
    first, second = column(routes[0:1]), column(routes[1:2])
    lanes = 128 * pl.cdiv(n_ep, 128)
    expert = lax.broadcasted_iota(jnp.int32, (tok, lanes), 1).astype(f32)
    is_first, is_second = expert == first, expert == second
    member = jnp.where(is_first, 1.0, 0.0) + jnp.where(is_second, 1.0, 0.0)
    earlier = jnp.where(
        lax.broadcasted_iota(jnp.int32, (tok, tok), 1)
        < lax.broadcasted_iota(jnp.int32, (tok, tok), 0),
        1.0,
        0.0,
    )
    before = jnp.dot(earlier.astype(bf16), member.astype(bf16), preferred_element_type=f32)
    place = before + expert * cap
    place_first = jnp.sum(jnp.where(is_first, place, 0.0), axis=1, keepdims=True)
    place_second = jnp.sum(jnp.where(is_second, place, 0.0), axis=1, keepdims=True)
    slots = lax.broadcasted_iota(jnp.int32, (tok, n_ep * cap), 1).astype(f32)
    at_first, at_second = slots == place_first, slots == place_second
    select = (jnp.where(at_first, 1.0, 0.0) + jnp.where(at_second, 1.0, 0.0)).astype(bf16)
    picked[...] = lax.dot_general(
        select, tokens_ref[...], (((0,), (0,)), ((), ())), preferred_element_type=f32
    ).astype(bf16)
    gains[pl.ds(tp, 1)] = in_gain_ref[...].astype(f32).reshape(1, 1, width)
    xall[pl.ds(tp, 1), my_rows] = picked[my_rows][None]

    pl.semaphore_wait(barrier, n_ep - 1 + n_tp - 1)

    dispatch = {
        d: remote(picked.at[rows[d]], xall.at[tp, my_rows], disp_s.at[d], disp_r.at[d], {"ep": source[d]})
        for d in range(1, n_ep)
    }
    to_partner, to_opposite, relay = [], [], []
    for d in range(n_ep):
        block = xall.at[tp, rows[d]]
        to_partner.append(remote(block, block, part_s.at[d], part_r.at[d], {"tp": partner}))
        to_opposite.append(remote(block, block, opp_s.at[d], opp_r.at[d], {"tp": opposite}))
        far = xall.at[opposite, rows[d]]
        relay.append(remote(far, far, rel_s.at[d], rel_r.at[d], {"tp": partner}))
    gain_copies = [
        remote(gains.at[tp], gains.at[tp], gain_s.at[i], gain_r.at[i], {"tp": peer})
        for i, peer in enumerate((partner, opposite, diagonal))
    ]
    for copy in gain_copies:
        copy.start()
    to_opposite[0].start()
    to_partner[0].start()
    order = near[1:]
    for d in order:
        dispatch[d].start()

    def forward(d):
        dispatch[d].wait_recv()
        to_opposite[d].start()
        to_partner[d].start()

    def pass_on(d):
        to_opposite[d].wait_recv()
        relay[d].start()

    def normalise(i, d):
        to_partner[d].wait_recv()
        relay[d].wait_recv()
        parts = [xall[j, rows[d]].astype(f32) for j in range(n_tp)]
        total = sum(jnp.sum(p * p, axis=1, keepdims=True) for p in parts)
        scale = lax.rsqrt(total / full + epsilon)
        for j in range(n_tp):
            xn[i * cap : (i + 1) * cap, j * width : (j + 1) * width] = (
                parts[j] * scale * gains[j]
            ).astype(bf16)

    tile = min(256, ff)
    tiles = ff // tile

    def units(h, start, stop):
        mine = slice(h * half_rows, (h + 1) * half_rows)

        def body(n, carry):
            cols = pl.ds(pl.multiple_of(n * tile, tile), tile)
            gate = jnp.dot(xn[mine], wg[:, cols], preferred_element_type=f32)
            up = jnp.dot(xn[mine], wu[:, cols], preferred_element_type=f32)
            hidden[mine, cols] = (gate / (1.0 + jnp.exp(-gate)) * up).astype(bf16)
            return carry

        lax.fori_loop(start, stop, body, 0)

    far_partner, near_partner = diagonal, partner
    partner_copies = {
        (h, k): remote(psend.at[h, k], prec.at[h, k], pd_s.at[h, k], pd_r.at[h, k], {"tp": partner})
        for h in range(2)
        for k in range(2)
    }

    def down(h):
        mine = slice(h * half_rows, (h + 1) * half_rows)

        def product(j):
            cols = pl.ds(pl.multiple_of(j * width, width), width)
            return jnp.dot(hidden[mine], wd[:, cols], preferred_element_type=f32)

        for k, j in enumerate((far_partner, near_partner)):
            psend[h, k] = product(j).astype(bf16)
            partner_copies[h, k].start()
        for k, j in enumerate((opposite, tp)):
            own[h, k] = product(j)

    across = [
        remote(xsend.at[i], xrec.at[i], xs_s.at[i], xs_r.at[i], {"tp": opposite})
        for i in range(n_ep)
    ]
    returned = {
        d: remote(rsend.at[d], back.at[my_rows], ret_s.at[d], ret_r.at[d], {"ep": source[d]})
        for d in range(1, n_ep)
    }

    def send_across(h):
        partner_copies[h, 0].wait_recv()
        for q in range(n_ep // 2):
            i = h * (n_ep // 2) + q
            part = slice(q * cap, (q + 1) * cap)
            xsend[i] = (own[h, 0, part] + prec[h, 0, part].astype(f32)).astype(bf16)
            across[i].start()

    def send_back(i):
        h, q = divmod(i, n_ep // 2)
        d = near[i]
        part = slice(q * cap, (q + 1) * cap)
        both = own[h, 1, part] + prec[h, 1, part].astype(f32)
        across[i].wait_recv()
        done = (both + xrec[i].astype(f32)).astype(bf16)
        if d == 0:
            back[my_rows] = done
        else:
            rsend[d] = done
            returned[d].start()

    half = n_ep // 2
    group_a, group_b = near[:half], near[half:]
    for copy in gain_copies:
        copy.wait_recv()
    for i in range(1, half):
        forward(group_a[i])
        pass_on(group_a[i - 1])
    pass_on(group_a[half - 1])
    for i, d in enumerate(group_a):
        normalise(i, d)
    for copy in weights[:2]:
        copy.wait()
    pieces = min(half, tiles)
    done = 0
    for piece in range(pieces):
        until = (piece + 1) * half // pieces
        for i in range(done, until):
            forward(group_b[i])
            if i:
                pass_on(group_b[i - 1])
        done = until
        units(0, piece * tiles // pieces, (piece + 1) * tiles // pieces)
    pass_on(group_b[half - 1])
    weights[2].wait()
    down(0)
    send_across(0)
    for i, d in enumerate(group_b):
        normalise(half + i, d)
    partner_copies[0, 1].wait_recv()
    done = 0
    for piece in range(pieces):
        units(1, piece * tiles // pieces, (piece + 1) * tiles // pieces)
        until = (piece + 1) * half // pieces
        for i in range(done, until):
            send_back(i)
        done = until
    down(1)
    send_across(1)
    partner_copies[1, 1].wait_recv()
    for i in range(half, n_ep):
        send_back(i)

    gates = gates_ref[...]
    mixing = jnp.where(at_first, column(gates[0:1]), 0.0) + jnp.where(
        at_second, column(gates[1:2]), 0.0
    )
    high = mixing.astype(bf16)
    low = (mixing - high.astype(f32)).astype(bf16)
    for d in range(1, n_ep):
        returned[d].wait_recv()
    rows_back = back[...]
    combined = jnp.dot(high, rows_back, preferred_element_type=f32) + jnp.dot(
        low, rows_back, preferred_element_type=f32
    )
    row_sum = jnp.sum(combined * combined, axis=1, keepdims=True)
    flat = jnp.sum(jnp.where(diag, row_sum, 0.0), axis=0, keepdims=True)
    sums[pl.ds(tp, 1)] = flat[None]
    norm_copies = [
        remote(sums.at[tp], sums.at[tp], ns_s.at[i], ns_r.at[i], {"tp": peer})
        for i, peer in enumerate((partner, opposite, diagonal))
    ]
    for copy in norm_copies:
        copy.start()

    for copy in gain_copies + to_partner + to_opposite + relay + across:
        copy.wait_send()
    for copies in (dispatch, partner_copies, returned):
        for copy in copies.values():
            copy.wait_send()

    for copy in norm_copies:
        copy.wait()
    total = sum(sums[j] for j in range(n_tp))
    scale = lax.rsqrt(column(total) / full + epsilon)
    gain = out_gain_ref[...].astype(f32).reshape(1, width)
    out_ref[...] = (combined * scale * gain).astype(bf16)


def fused(tokens, norm_gain, routes, gate_weights, w_gate, w_up, w_down, out_gain):
    n_ep, n_tp = lax.axis_size("ep"), lax.axis_size("tp")
    tok, width = tokens.shape
    cap = 2 * routes.shape[1] * tok // n_ep
    _, d_model, ff = w_gate.shape
    half_rows = n_ep // 2 * cap
    near = tuple(range(0, n_ep, 2)) + tuple(range(1, n_ep, 2))
    bf16, f32 = jnp.bfloat16, jnp.float32
    dma = pltpu.SemaphoreType.DMA
    vmem = pl.BlockSpec(memory_space=pltpu.VMEM)
    anywhere = pl.BlockSpec(memory_space=pl.ANY)
    slots = n_ep * cap
    return pl.pallas_call(
        functools.partial(layer, n_ep, cap, near),
        out_shape=jax.ShapeDtypeStruct((tok, width), bf16),
        in_specs=[vmem] * 5 + [anywhere] * 3,
        out_specs=vmem,
        scratch_shapes=[
            pltpu.VMEM((d_model, ff), bf16),
            pltpu.VMEM((d_model, ff), bf16),
            pltpu.VMEM((ff, d_model), bf16),
            pltpu.VMEM((slots, width), bf16),
            pltpu.VMEM((n_tp, slots, width), bf16),
            pltpu.VMEM((n_tp, 1, width), f32),
            pltpu.VMEM((slots, d_model), bf16),
            pltpu.VMEM((slots, ff), bf16),
            pltpu.VMEM((2, 2, half_rows, width), bf16),
            pltpu.VMEM((2, 2, half_rows, width), bf16),
            pltpu.VMEM((2, 2, half_rows, width), f32),
            pltpu.VMEM((n_ep, cap, width), bf16),
            pltpu.VMEM((n_ep, cap, width), bf16),
            pltpu.VMEM((n_ep, cap, width), bf16),
            pltpu.VMEM((slots, width), bf16),
            pltpu.VMEM((n_tp, 1, tok), f32),
            dma((3,)),
            *[dma((n_ep,))] * 8,
            *[dma((3,))] * 2,
            *[dma((2, 2))] * 2,
            *[dma((n_ep,))] * 4,
            *[dma((3,))] * 2,
        ],
        compiler_params=pltpu.CompilerParams(
            collective_id=0, has_side_effects=True, vmem_limit_bytes=60 * 1024 * 1024
        ),
    )(
        routes.T, gate_weights.T, tokens, norm_gain, out_gain,
        w_gate, w_up, w_down,
    )


def solution(mesh):
    placed = (
        P("ep", "tp"),
        P("tp"),
        P("ep", None),
        P("ep", None),
        P("ep", None, "tp"),
        P("ep", None, "tp"),
        P("ep", "tp", None),
        P("tp"),
    )
    n_ep = mesh.shape["ep"]
    pairs = mesh.shape["tp"] == 2 * CORES and n_ep >= 8 and n_ep & (n_ep - 1) == 0
    return jax.shard_map(
        fused if pairs else shards, mesh=mesh, in_specs=placed, out_specs=P("ep", "tp"), check_vma=False
    )
```

```python
import functools

import jax
import jax.numpy as jnp
from jax import lax
from jax.experimental import pallas as pl
from jax.experimental.pallas import tpu as pltpu
from jax.sharding import PartitionSpec as P

epsilon = 1e-06
CORES = 2


def shards(tokens, norm_gain, routes, gate_weights, w_gate, w_up, w_down, out_gain):
    tok_rows = tokens.shape[0]
    width_local = tokens.shape[1]
    full_width = width_local * lax.axis_size("tp")
    experts = lax.axis_size("ep")
    top_count = routes.shape[1]
    capacity = 2 * top_count * tok_rows // experts
    flat_ids = routes.reshape(-1)
    onehot = (flat_ids[:, None] == jnp.arange(experts, dtype=jnp.int32)[None, :]).astype(jnp.int32)
    before = jnp.cumsum(onehot, axis=0) - onehot
    slot_index = jnp.sum(before * onehot, axis=1)
    dest_index = flat_ids * capacity + slot_index
    dest_pairs = dest_index.reshape(tok_rows, top_count)
    places = jnp.arange(experts * capacity, dtype=jnp.int32)
    scatter_mat = jnp.any(dest_pairs[None, :, :] == places[:, None, None], axis=2).astype(
        jnp.bfloat16
    )
    gate_mat = w_gate[0]
    up_mat = w_up[0]
    x_float = tokens.astype(jnp.float32)
    row_sums = lax.psum(jnp.sum(x_float * x_float, axis=1), "tp")
    scale_in = lax.rsqrt(row_sums / full_width + epsilon)
    normed = (x_float * scale_in[:, None] * norm_gain.astype(jnp.float32)).astype(jnp.bfloat16)
    outgoing = jnp.dot(scatter_mat, normed, preferred_element_type=jnp.float32).astype(jnp.bfloat16)
    arrived = lax.all_to_all(outgoing, "ep", split_axis=0, concat_axis=0, tiled=True)
    portion = lax.all_gather(arrived, "tp", axis=1, tiled=True)
    gate_sum = jnp.dot(portion, gate_mat, preferred_element_type=jnp.float32)
    up_sum = jnp.dot(portion, up_mat, preferred_element_type=jnp.float32)
    hidden = (jax.nn.silu(gate_sum) * up_sum).astype(jnp.bfloat16)
    down_mat = w_down[0]
    summed = lax.psum_scatter(
        lax.dot_general(
            down_mat, hidden, (((0,), (1,)), ((), ())), preferred_element_type=jnp.float32
        ).astype(jnp.bfloat16),
        "tp",
        scatter_dimension=0,
        tiled=True,
    )
    came_back = lax.all_to_all(summed, "ep", split_axis=1, concat_axis=1, tiled=True)
    picked = (
        jnp.take(came_back, dest_index, axis=1)
        .astype(jnp.float32)
        .reshape(width_local, tok_rows, top_count)
    )
    combined = jnp.sum(picked * gate_weights[None, :, :], axis=2).T
    out_sums = lax.psum(jnp.sum(combined * combined, axis=1), "tp")
    scale_out = lax.rsqrt(out_sums / full_width + epsilon)
    return (combined * scale_out[:, None] * out_gain.astype(jnp.float32)).astype(jnp.bfloat16)


def xor(index, mask):
    result = index
    bit = 1
    while bit <= mask:
        if mask & bit:
            result = result + bit * (1 - 2 * ((index // bit) % 2))
        bit *= 2
    return result


def layer(
    n_ep, cap, near,
    routes_ref, gates_ref, tokens_ref, in_gain_ref, out_gain_ref, wg_hbm, wu_hbm, wd_hbm,
    out_ref,
    wg, wu, wd, picked, xall, gains, xn, hidden, psend, prec, own, xsend, xrec, rsend, back, sums,
    w_sem, disp_s, disp_r, part_s, part_r, opp_s, opp_r, rel_s, rel_r, gain_s, gain_r,
    pd_s, pd_r, xs_s, xs_r, ret_s, ret_r, ns_s, ns_r,
):
    f32, bf16 = jnp.float32, jnp.bfloat16
    ep, tp = lax.axis_index("ep"), lax.axis_index("tp")
    chip, core = tp // CORES, tp % CORES
    partner = chip * CORES + (1 - core)
    opposite = (1 - chip) * CORES + core
    diagonal = (1 - chip) * CORES + (1 - core)
    tok, width = tokens_ref.shape
    n_tp = gains.shape[0]
    full = width * n_tp
    ff = wg.shape[1]
    half_rows = n_ep // 2 * cap
    source = [xor(ep, d) for d in range(n_ep)]
    rows = [pl.ds(pl.multiple_of(s * cap, cap), cap) for s in source]
    my_rows = rows[0]

    barrier = pltpu.get_barrier_semaphore()
    for d in range(1, n_ep):
        pl.semaphore_signal(barrier, inc=1, device_id={"ep": source[d]})
    for peer in (partner, opposite, diagonal):
        pl.semaphore_signal(barrier, inc=1, device_id={"tp": peer})

    weights = [
        pltpu.make_async_copy(src.at[0], dst, w_sem.at[i])
        for i, (src, dst) in enumerate(((wg_hbm, wg), (wu_hbm, wu), (wd_hbm, wd)))
    ]
    for copy in weights:
        copy.start()

    def remote(src, dst, send, recv, where):
        return pltpu.make_async_remote_copy(
            src_ref=src, dst_ref=dst, send_sem=send, recv_sem=recv, device_id=where
        )

    diag = lax.broadcasted_iota(jnp.int32, (tok, tok), 0) == lax.broadcasted_iota(
        jnp.int32, (tok, tok), 1
    )

    def column(row):
        return jnp.sum(jnp.where(diag, row, 0.0), axis=1, keepdims=True)

    routes = routes_ref[...].astype(f32)
    first, second = column(routes[0:1]), column(routes[1:2])
    lanes = 128 * pl.cdiv(n_ep, 128)
    expert = lax.broadcasted_iota(jnp.int32, (tok, lanes), 1).astype(f32)
    is_first, is_second = expert == first, expert == second
    member = jnp.where(is_first, 1.0, 0.0) + jnp.where(is_second, 1.0, 0.0)
    earlier = jnp.where(
        lax.broadcasted_iota(jnp.int32, (tok, tok), 1)
        < lax.broadcasted_iota(jnp.int32, (tok, tok), 0),
        1.0,
        0.0,
    )
    before = jnp.dot(earlier.astype(bf16), member.astype(bf16), preferred_element_type=f32)
    place = before + expert * cap
    place_first = jnp.sum(jnp.where(is_first, place, 0.0), axis=1, keepdims=True)
    place_second = jnp.sum(jnp.where(is_second, place, 0.0), axis=1, keepdims=True)
    slots = lax.broadcasted_iota(jnp.int32, (tok, n_ep * cap), 1).astype(f32)
    at_first, at_second = slots == place_first, slots == place_second
    select = (jnp.where(at_first, 1.0, 0.0) + jnp.where(at_second, 1.0, 0.0)).astype(bf16)
    picked[...] = lax.dot_general(
        select, tokens_ref[...], (((0,), (0,)), ((), ())), preferred_element_type=f32
    ).astype(bf16)
    gains[pl.ds(tp, 1)] = in_gain_ref[...].astype(f32).reshape(1, 1, width)
    xall[pl.ds(tp, 1), my_rows] = picked[my_rows][None]

    pl.semaphore_wait(barrier, n_ep - 1 + n_tp - 1)

    dispatch = {
        d: remote(picked.at[rows[d]], xall.at[tp, my_rows], disp_s.at[d], disp_r.at[d], {"ep": source[d]})
        for d in range(1, n_ep)
    }
    to_partner, to_opposite, relay = [], [], []
    for d in range(n_ep):
        block = xall.at[tp, rows[d]]
        to_partner.append(remote(block, block, part_s.at[d], part_r.at[d], {"tp": partner}))
        to_opposite.append(remote(block, block, opp_s.at[d], opp_r.at[d], {"tp": opposite}))
        far = xall.at[opposite, rows[d]]
        relay.append(remote(far, far, rel_s.at[d], rel_r.at[d], {"tp": partner}))
    gain_copies = [
        remote(gains.at[tp], gains.at[tp], gain_s.at[i], gain_r.at[i], {"tp": peer})
        for i, peer in enumerate((partner, opposite, diagonal))
    ]
    for copy in gain_copies:
        copy.start()
    to_opposite[0].start()
    to_partner[0].start()
    order = near[1:]
    for d in order:
        dispatch[d].start()

    def forward(d):
        dispatch[d].wait_recv()
        to_opposite[d].start()
        to_partner[d].start()

    def pass_on(d):
        to_opposite[d].wait_recv()
        relay[d].start()

    def normalise(i, d):
        to_partner[d].wait_recv()
        relay[d].wait_recv()
        parts = [xall[j, rows[d]].astype(f32) for j in range(n_tp)]
        total = sum(jnp.sum(p * p, axis=1, keepdims=True) for p in parts)
        scale = lax.rsqrt(total / full + epsilon)
        for j in range(n_tp):
            xn[i * cap : (i + 1) * cap, j * width : (j + 1) * width] = (
                parts[j] * scale * gains[j]
            ).astype(bf16)

    tile = min(256, ff)
    tiles = ff // tile

    def units(h, start, stop):
        mine = slice(h * half_rows, (h + 1) * half_rows)

        def body(n, carry):
            cols = pl.ds(pl.multiple_of(n * tile, tile), tile)
            gate = jnp.dot(xn[mine], wg[:, cols], preferred_element_type=f32)
            up = jnp.dot(xn[mine], wu[:, cols], preferred_element_type=f32)
            hidden[mine, cols] = (gate / (1.0 + jnp.exp(-gate)) * up).astype(bf16)
            return carry

        lax.fori_loop(start, stop, body, 0)

    far_partner, near_partner = diagonal, partner
    partner_copies = {
        (h, k): remote(psend.at[h, k], prec.at[h, k], pd_s.at[h, k], pd_r.at[h, k], {"tp": partner})
        for h in range(2)
        for k in range(2)
    }

    def down(h):
        mine = slice(h * half_rows, (h + 1) * half_rows)

        def product(j):
            cols = pl.ds(pl.multiple_of(j * width, width), width)
            return jnp.dot(hidden[mine], wd[:, cols], preferred_element_type=f32)

        for k, j in enumerate((far_partner, near_partner)):
            psend[h, k] = product(j).astype(bf16)
            partner_copies[h, k].start()
        for k, j in enumerate((opposite, tp)):
            own[h, k] = product(j)

    across = [
        remote(xsend.at[i], xrec.at[i], xs_s.at[i], xs_r.at[i], {"tp": opposite})
        for i in range(n_ep)
    ]
    returned = {
        d: remote(rsend.at[d], back.at[my_rows], ret_s.at[d], ret_r.at[d], {"ep": source[d]})
        for d in range(1, n_ep)
    }

    def send_across(h):
        partner_copies[h, 0].wait_recv()
        for q in range(n_ep // 2):
            i = h * (n_ep // 2) + q
            part = slice(q * cap, (q + 1) * cap)
            xsend[i] = (own[h, 0, part] + prec[h, 0, part].astype(f32)).astype(bf16)
            across[i].start()

    def send_back(i):
        h, q = divmod(i, n_ep // 2)
        d = near[i]
        part = slice(q * cap, (q + 1) * cap)
        both = own[h, 1, part] + prec[h, 1, part].astype(f32)
        across[i].wait_recv()
        done = (both + xrec[i].astype(f32)).astype(bf16)
        if d == 0:
            back[my_rows] = done
        else:
            rsend[d] = done
            returned[d].start()

    half = n_ep // 2
    group_a, group_b = near[:half], near[half:]
    for copy in gain_copies:
        copy.wait_recv()
    for i in range(1, half):
        forward(group_a[i])
    for d in group_a:
        pass_on(d)
    for i, d in enumerate(group_a):
        normalise(i, d)
    for copy in weights[:2]:
        copy.wait()
    pieces = min(half, tiles)
    done = 0
    for piece in range(pieces):
        until = (piece + 1) * half // pieces
        for i in range(done, until):
            forward(group_b[i])
            if i:
                pass_on(group_b[i - 1])
        done = until
        units(0, piece * tiles // pieces, (piece + 1) * tiles // pieces)
    pass_on(group_b[half - 1])
    weights[2].wait()
    down(0)
    send_across(0)
    for i, d in enumerate(group_b):
        normalise(half + i, d)
    partner_copies[0, 1].wait_recv()
    done = 0
    for piece in range(pieces):
        units(1, piece * tiles // pieces, (piece + 1) * tiles // pieces)
        until = (piece + 1) * half // pieces
        for i in range(done, until):
            send_back(i)
        done = until
    down(1)
    send_across(1)
    partner_copies[1, 1].wait_recv()
    for i in range(half, n_ep):
        send_back(i)

    gates = gates_ref[...]
    mixing = jnp.where(at_first, column(gates[0:1]), 0.0) + jnp.where(
        at_second, column(gates[1:2]), 0.0
    )
    high = mixing.astype(bf16)
    low = (mixing - high.astype(f32)).astype(bf16)
    for d in range(1, n_ep):
        returned[d].wait_recv()
    rows_back = back[...]
    combined = jnp.dot(high, rows_back, preferred_element_type=f32) + jnp.dot(
        low, rows_back, preferred_element_type=f32
    )
    row_sum = jnp.sum(combined * combined, axis=1, keepdims=True)
    flat = jnp.sum(jnp.where(diag, row_sum, 0.0), axis=0, keepdims=True)
    sums[pl.ds(tp, 1)] = flat[None]
    norm_copies = [
        remote(sums.at[tp], sums.at[tp], ns_s.at[i], ns_r.at[i], {"tp": peer})
        for i, peer in enumerate((partner, opposite, diagonal))
    ]
    for copy in norm_copies:
        copy.start()

    for copy in gain_copies + to_partner + to_opposite + relay + across:
        copy.wait_send()
    for copies in (dispatch, partner_copies, returned):
        for copy in copies.values():
            copy.wait_send()

    for copy in norm_copies:
        copy.wait()
    total = sum(sums[j] for j in range(n_tp))
    scale = lax.rsqrt(column(total) / full + epsilon)
    gain = out_gain_ref[...].astype(f32).reshape(1, width)
    out_ref[...] = (combined * scale * gain).astype(bf16)


def fused(tokens, norm_gain, routes, gate_weights, w_gate, w_up, w_down, out_gain):
    n_ep, n_tp = lax.axis_size("ep"), lax.axis_size("tp")
    tok, width = tokens.shape
    cap = 2 * routes.shape[1] * tok // n_ep
    _, d_model, ff = w_gate.shape
    half_rows = n_ep // 2 * cap
    near = tuple(range(0, n_ep, 2)) + tuple(range(1, n_ep, 2))
    bf16, f32 = jnp.bfloat16, jnp.float32
    dma = pltpu.SemaphoreType.DMA
    vmem = pl.BlockSpec(memory_space=pltpu.VMEM)
    anywhere = pl.BlockSpec(memory_space=pl.ANY)
    slots = n_ep * cap
    return pl.pallas_call(
        functools.partial(layer, n_ep, cap, near),
        out_shape=jax.ShapeDtypeStruct((tok, width), bf16),
        in_specs=[vmem] * 5 + [anywhere] * 3,
        out_specs=vmem,
        scratch_shapes=[
            pltpu.VMEM((d_model, ff), bf16),
            pltpu.VMEM((d_model, ff), bf16),
            pltpu.VMEM((ff, d_model), bf16),
            pltpu.VMEM((slots, width), bf16),
            pltpu.VMEM((n_tp, slots, width), bf16),
            pltpu.VMEM((n_tp, 1, width), f32),
            pltpu.VMEM((slots, d_model), bf16),
            pltpu.VMEM((slots, ff), bf16),
            pltpu.VMEM((2, 2, half_rows, width), bf16),
            pltpu.VMEM((2, 2, half_rows, width), bf16),
            pltpu.VMEM((2, 2, half_rows, width), f32),
            pltpu.VMEM((n_ep, cap, width), bf16),
            pltpu.VMEM((n_ep, cap, width), bf16),
            pltpu.VMEM((n_ep, cap, width), bf16),
            pltpu.VMEM((slots, width), bf16),
            pltpu.VMEM((n_tp, 1, tok), f32),
            dma((3,)),
            *[dma((n_ep,))] * 8,
            *[dma((3,))] * 2,
            *[dma((2, 2))] * 2,
            *[dma((n_ep,))] * 4,
            *[dma((3,))] * 2,
        ],
        compiler_params=pltpu.CompilerParams(
            collective_id=0, has_side_effects=True, vmem_limit_bytes=60 * 1024 * 1024
        ),
    )(
        routes.T, gate_weights.T, tokens, norm_gain, out_gain,
        w_gate, w_up, w_down,
    )


def solution(mesh):
    placed = (
        P("ep", "tp"),
        P("tp"),
        P("ep", None),
        P("ep", None),
        P("ep", None, "tp"),
        P("ep", None, "tp"),
        P("ep", "tp", None),
        P("tp"),
    )
    n_ep = mesh.shape["ep"]
    pairs = mesh.shape["tp"] == 2 * CORES and n_ep >= 8 and n_ep & (n_ep - 1) == 0
    return jax.shard_map(
        fused if pairs else shards, mesh=mesh, in_specs=placed, out_specs=P("ep", "tp"), check_vma=False
    )
```
